32 devices in a mesh: grp: 2 (over y), sp: 4 (over z), dp: 4 (over x, core).
Axes of the slice: x: 2, y: 2, z: 4, core: 2. Of those that a mesh axis runs over, the one named last changes fastest.
Arguments:
- tokens: bfloat16 [8, 640, 2048], P(('grp', 'dp'), 'sp'), parts along dimension 0, may hold values from -6 to 6
- query_weight: bfloat16 [2048, 1024], P('dp'), may hold values from -0.125 to 0.125
- key_weight: bfloat16 [2048, 256], P('dp'), may hold values from -0.125 to 0.125
- value_weight: bfloat16 [2048, 256], P('dp'), may hold values from -0.125 to 0.125
- out_weight: bfloat16 [1024, 2048], P(None, 'dp'), may hold values from -0.1875 to 0.1875
- query_gain: float32 [64], replicated, may hold values from 0.28 to 6
- key_gain: float32 [64], replicated, may hold values from 0.28 to 6
Outputs:
- mixed: bfloat16 [8, 640, 2048], P(('grp', 'dp'), 'sp'), parts along dimension 0
The draws below stay inside these ranges and needn't reach their ends.
There are 2 independent parts, one for each index of `grp`. The reference program is written for one: setup_inputs(seed, part) draws one part's arguments, and reference() takes and returns one part's arrays. A program takes and returns all parts, laid end to end along the dimension named above; an argument that names none is the same for every part. Nothing has to cross between parts.
All inputs are finite; a program needn't handle non-finite values.
Results may differ from the reference program's by a relative error of at most 0.006.
The reference program's roundings to bfloat16 on the way count: a program that leaves them out, or rounds other values in their place, can miss the bound.
Values may be sent and summed in bfloat16 or wider, within the bound.
No kernel may reach another device: no remote copies, remote signals or barrier semaphores. Data moves between devices by JAX's collectives and lax.ppermute only.
A program may use at most 64 MiB of HBM per device.

```python
import jax
import jax.numpy as jnp
from jax import lax

D = 2048
HEADS = 16
KV_HEADS = 4
HEAD_DIM = 64
GRID_W = 64
SEQ_LEN = 640
SEQS = 4


def gain_values(key):
    return 1.0 + 0.18 * jnp.clip(jax.random.normal(key, (HEAD_DIM,), jnp.float32), -4.0, 4.0)


def draw_query_gain(key, part):
    return gain_values(jax.random.fold_in(key, 11))


def draw_key_gain(key, part):
    return gain_values(jax.random.fold_in(key, 23))


def level_of(rng, dims, split, least, largest):
    factor_of, own = 1.0, jax.random.fold_in(rng, 6)
    for position, blocks in split:
        steps = jnp.exp(jax.random.uniform(jax.random.fold_in(own, position), (blocks,), jnp.float32, least / len(split), largest / len(split)))
        factor_of = factor_of * jnp.repeat(steps, dims[position] // blocks).reshape([-1 if axis == position else 1 for axis in range(len(dims))])
    return factor_of


def gaussian(rng, shape, spread, bound, pieces=(), kind=jnp.bfloat16):
    values = jax.random.normal(rng, shape, jnp.float32) * spread
    if len(pieces) > 0:
        values = level_of(rng, shape, pieces, -0.22, 0.18) * values
    return jnp.clip(values, min=-bound, max=bound).astype(kind)


def setup_inputs(seed: int = 0, part: int = 0) -> dict:
    splits = jax.random.split(jax.random.key(seed), 8)
    part_splits = jax.random.split(jax.random.fold_in(splits[7], part), 8)
    tokens = gaussian(part_splits[0], (SEQS, SEQ_LEN, D), 1.0, 6.0, ((0, 4), (1, 4)))
    query_weight = gaussian(splits[1], (D, HEADS * HEAD_DIM), D ** -0.5, 0.125, ((0, 4),))
    key_weight = gaussian(splits[2], (D, KV_HEADS * HEAD_DIM), D ** -0.5, 0.125, ((0, 4),))
    value_weight = gaussian(splits[3], (D, KV_HEADS * HEAD_DIM), D ** -0.5, 0.125, ((0, 4),))
    out_weight = gaussian(splits[4], (HEADS * HEAD_DIM, D), (HEADS * HEAD_DIM) ** -0.5, 0.1875, ((1, 4),))
    query_gain = draw_query_gain(jax.random.fold_in(splits[7], 71), part)
    key_gain = draw_key_gain(jax.random.fold_in(splits[7], 71), part)
    return dict(tokens=tokens, query_weight=query_weight, key_weight=key_weight, value_weight=value_weight, out_weight=out_weight, query_gain=query_gain, key_gain=key_gain)


theta_base = 10000.0
norm_eps = 1e-06

def rotary_tables(positions):
    quarter = HEAD_DIM // 4
    inverse = theta_base ** (-jnp.arange(quarter, dtype=jnp.float32) / quarter)
    grid_rows = (positions // GRID_W).astype(jnp.float32)
    grid_cols = (positions % GRID_W).astype(jnp.float32)
    angles = jnp.concatenate([grid_rows[:, None] * inverse, grid_cols[:, None] * inverse], axis=-1)
    return (jnp.cos(angles), jnp.sin(angles))

def norm_rotate(raw, gain, cosine, sine):
    scaled = raw * lax.rsqrt(lax.optimization_barrier(jnp.mean(raw * raw, axis=-1, keepdims=True)) + norm_eps) * gain
    half = HEAD_DIM // 2
    first_half = scaled[..., :half]
    second_half = scaled[..., half:]
    cosine = cosine[:, None, :]
    sine = sine[:, None, :]
    turned = jnp.concatenate([first_half * cosine - second_half * sine, second_half * cosine + first_half * sine], axis=-1)
    return turned.astype(jnp.bfloat16)

def reference(tokens, query_weight, key_weight, value_weight, out_weight, query_gain, key_gain):
    length = tokens.shape[1]
    per_kv = HEADS // KV_HEADS
    cosine, sine = rotary_tables(jnp.arange(length, dtype=jnp.int32))
    scale = HEAD_DIM ** (-0.5)

    def one_sequence(rows_in):
        raw_q = jnp.dot(rows_in, query_weight, preferred_element_type=jnp.float32).reshape(length, HEADS, HEAD_DIM)
        raw_k = jnp.dot(rows_in, key_weight, preferred_element_type=jnp.float32).reshape(length, KV_HEADS, HEAD_DIM)
        values = jnp.dot(rows_in, value_weight, preferred_element_type=jnp.float32).astype(jnp.bfloat16)
        queries = norm_rotate(raw_q, query_gain, cosine, sine)
        keys = norm_rotate(raw_k, key_gain, cosine, sine)
        query_heads = queries.reshape(length, KV_HEADS, per_kv, HEAD_DIM).transpose(1, 0, 2, 3)
        key_heads = keys.transpose(1, 0, 2)
        value_heads = values.reshape(length, KV_HEADS, HEAD_DIM).transpose(1, 0, 2)

        def one_head(operands):
            head_q, head_k, head_v = operands
            scores = jnp.einsum('qgd,sd->gqs', head_q.astype(jnp.float32), head_k.astype(jnp.float32)) * scale
            top = lax.optimization_barrier(jnp.max(scores, axis=-1, keepdims=True))
            weights = jnp.exp(scores - top)
            probs = (weights / lax.optimization_barrier(jnp.sum(weights, axis=-1, keepdims=True))).astype(jnp.bfloat16)
            return jnp.einsum('gqs,sd->qgd', probs.astype(jnp.float32), head_v.astype(jnp.float32)).astype(jnp.bfloat16)
        attended = lax.map(one_head, (query_heads, key_heads, value_heads))
        attended = attended.transpose(1, 0, 2, 3).reshape(length, HEADS * HEAD_DIM)
        return jnp.dot(attended, out_weight, preferred_element_type=jnp.float32).astype(jnp.bfloat16)
    return lax.map(one_sequence, tokens)
```

```python
import functools

import jax
import jax.numpy as jnp
from jax import lax
from jax.experimental import pallas as pl
from jax.experimental.pallas import tpu as pltpu
from jax.sharding import PartitionSpec as P

HEADS = 16
KV_HEADS = 4
HEAD_DIM = 64
GRID_W = 64
LANES = 128


theta_base = 10000.0
norm_eps = 1e-06
F32 = jnp.float32
BF16 = jnp.bfloat16
VMEM = pl.BlockSpec(memory_space=pltpu.VMEM)


def rotary_tables(positions, gain):
    quarter = HEAD_DIM // 4
    half = HEAD_DIM // 2
    inverse = theta_base ** (-jnp.arange(quarter, dtype=F32) / quarter)
    grid_rows = (positions // GRID_W).astype(F32)
    grid_cols = (positions % GRID_W).astype(F32)
    angles = jnp.concatenate([grid_rows[:, None] * inverse, grid_cols[:, None] * inverse], axis=-1)
    cosine, sine = jnp.cos(angles), jnp.sin(angles)
    first, second = gain[:half], gain[half:]
    straight = jnp.concatenate([cosine * first, cosine * second] * 2, axis=-1)
    crossed = jnp.concatenate([-sine * second, sine * first] * 2, axis=-1)
    return straight, crossed


def head_mean_matrix(width):
    rows = lax.broadcasted_iota(jnp.int32, (width, width), 0) // HEAD_DIM
    cols = lax.broadcasted_iota(jnp.int32, (width, width), 1) // HEAD_DIM
    return jnp.where(rows == cols, 1.0 / HEAD_DIM, 0.0).astype(BF16)


def norm_rotate(raw, straight, crossed):
    width = raw.shape[1]
    square = raw * raw
    high = square.astype(BF16)
    low = (square - high.astype(F32)).astype(BF16)
    averager = head_mean_matrix(width)
    mean = jnp.dot(high, averager, preferred_element_type=F32)
    mean += jnp.dot(low, averager, preferred_element_type=F32)
    factor = lax.rsqrt(mean + norm_eps)
    half = HEAD_DIM // 2
    lane = lax.broadcasted_iota(jnp.int32, (raw.shape[0], LANES), 1)
    is_first = lane % HEAD_DIM < half
    out = []
    for start in range(0, width, LANES):
        u = raw[:, start : start + LANES]
        swapped = jnp.where(is_first, pltpu.roll(u, LANES - half, 1), pltpu.roll(u, half, 1))
        out.append((u * straight + swapped * crossed) * factor[:, start : start + LANES])
    return out


def project(x_ref, shard_ref, refs, block_cols, width):
    total = None
    for index, ref, start in block_cols:
        rows = ref.shape[0]
        x = x_ref[:, pl.ds(pl.multiple_of(index * rows, LANES), rows)]
        w = ref[...] if start is None else ref[:, pl.ds(pl.multiple_of(start, LANES), width)]
        part = jnp.dot(x, w, preferred_element_type=F32)
        total = part if total is None else total + part
    return total


def projection_kernel(plan, rotate, width, place_ref, x_ref, *refs):
    n_weights = max(item[0] for _, items in plan for item in items) + 1
    weights = refs[:n_weights]
    out_ref = refs[-1]
    for out_slot, items in plan:
        sources = [
            (place_ref[shard], weights[number], None if start is None else place_ref[start])
            for number, shard, start in items
        ]
        raw = project(x_ref, None, None, sources, width)
        if rotate:
            straight, crossed = refs[n_weights][...], refs[n_weights + 1][...]
            parts = norm_rotate(raw, straight, crossed)
        else:
            parts = [raw[:, s : s + LANES] for s in range(0, width, LANES)]
        base = place_ref[out_slot]
        for number, part in enumerate(parts):
            at = pl.multiple_of(base + number * LANES, LANES)
            out_ref[:, pl.ds(at, LANES)] = part.astype(out_ref.dtype)


def run_projection(x, places, blocks, width, columns, tables, name):
    slots, values, arrays, plan = {}, [], [], []

    def slot_of(value):
        values.append(value)
        return len(values) - 1

    for out_start, items in blocks:
        row = []
        for piece, shard, start in items:
            found = [k for k, a in enumerate(arrays) if a is piece]
            if not found:
                arrays.append(piece)
                found = [len(arrays) - 1]
            row.append((found[0], slot_of(shard), None if start is None else slot_of(start)))
        plan.append((slot_of(out_start), row))
    place = jnp.stack([jnp.asarray(v, jnp.int32) for v in values])
    operands = [x, *arrays, *(tables or ())]
    flops = 2 * x.shape[0] * x.shape[1] * width * len(blocks)
    return pl.pallas_call(
        functools.partial(projection_kernel, plan, tables is not None, width),
        out_shape=jax.ShapeDtypeStruct((x.shape[0], columns), BF16),
        in_specs=[pl.BlockSpec(memory_space=pltpu.SMEM)] + [VMEM] * len(operands),
        out_specs=VMEM,
        compiler_params=pltpu.CompilerParams(vmem_limit_bytes=24 * 2**20),
        cost_estimate=pl.CostEstimate(flops=flops, bytes_accessed=flops // 200, transcendentals=0),
        name=name,
    )(place, *operands)


def attention_kernel(n_blocks, q_ref, *refs):
    k_refs, v_refs, out_ref = refs[:n_blocks], refs[n_blocks : 2 * n_blocks], refs[-1]
    rows = q_ref.shape[0]
    per_kv = HEADS // KV_HEADS
    scale = HEAD_DIM ** (-0.5) * 1.4426950408889634

    def doubled(refs_, head):
        start = head * HEAD_DIM // LANES * LANES
        tile = jnp.concatenate([r[:, start : start + LANES] for r in refs_], axis=0).astype(F32)
        other = pltpu.roll(tile, HEAD_DIM, 1)
        lane = lax.broadcasted_iota(jnp.int32, tile.shape, 1)
        lower = (lane < HEAD_DIM) == (head * HEAD_DIM % LANES == 0)
        return jnp.where(lower, tile, other).astype(BF16)

    lane = lax.broadcasted_iota(jnp.int32, (rows, LANES), 1)
    for head in range(KV_HEADS):
        keys = doubled(k_refs, head)
        values = doubled(v_refs, head)
        values = jnp.concatenate([values, jnp.ones(values.shape, BF16)], axis=1)
        for pair in range(per_kv // 2):
            start = (head * per_kv + pair * 2) * HEAD_DIM
            q = q_ref[:, start : start + LANES]
            halves = []
            for low in (True, False):
                masked = jnp.where((lane < HEAD_DIM) == low, q, jnp.zeros_like(q))
                scores = lax.dot_general(
                    masked, keys, (((1,), (1,)), ((), ())), preferred_element_type=F32
                )
                top = jnp.max(scores, axis=-1, keepdims=True)
                probs = jnp.exp2((scores - top) * scale).astype(BF16)
                both = jnp.dot(probs, values, preferred_element_type=F32)
                halves.append(both[:, :LANES] / both[:, LANES:])
            out_ref[:, start : start + LANES] = jnp.where(
                lane < HEAD_DIM, halves[0], halves[1]
            ).astype(BF16)


def attend(q, keys, values):
    rows, length = q.shape[0], q.shape[0] * len(keys)
    flops = 4 * rows * length * HEADS * HEAD_DIM
    return pl.pallas_call(
        functools.partial(attention_kernel, len(keys)),
        out_shape=jax.ShapeDtypeStruct(q.shape, BF16),
        in_specs=[VMEM] * (1 + 2 * len(keys)),
        out_specs=VMEM,
        compiler_params=pltpu.CompilerParams(vmem_limit_bytes=24 * 2**20),
        cost_estimate=pl.CostEstimate(
            flops=flops, bytes_accessed=4 * 2**20, transcendentals=rows * length * HEADS
        ),
        name="attend",
    )(q, *keys, *values)


def out_kernel(n_pieces, place_ref, a_ref, *refs):
    out_ref = refs[-1]
    a = a_ref[...]
    for number in range(n_pieces):
        piece = refs[number]
        width = piece.shape[1]
        result = jnp.dot(a, piece[...], preferred_element_type=F32)
        at = pl.multiple_of(place_ref[number], LANES)
        out_ref[:, pl.ds(at, width)] = result.astype(BF16)


def project_out(attended, pieces, columns):
    rows = attended.shape[0]
    place = jnp.stack([jnp.asarray(start, jnp.int32) for _, start in pieces])
    flops = 2 * rows * attended.shape[1] * columns
    return pl.pallas_call(
        functools.partial(out_kernel, len(pieces)),
        out_shape=jax.ShapeDtypeStruct((rows, columns), BF16),
        in_specs=[pl.BlockSpec(memory_space=pltpu.SMEM)] + [VMEM] * (1 + len(pieces)),
        out_specs=VMEM,
        compiler_params=pltpu.CompilerParams(vmem_limit_bytes=24 * 2**20),
        cost_estimate=pl.CostEstimate(flops=flops, bytes_accessed=flops // 100, transcendentals=0),
        name="project_out",
    )(place, attended, *[piece for piece, _ in pieces])


def layer(sizes, tokens, query_weight, key_weight, value_weight, out_weight, query_gain, key_gain):
    groups, parts, shards = sizes
    rows = tokens.shape[1]
    x = tokens.reshape(rows, tokens.shape[2])
    group, part, shard = lax.axis_index("grp"), lax.axis_index("sp"), lax.axis_index("dp")

    def shift(value, axis, size, by):
        return lax.ppermute(value, axis, [(i, (i + by) % size) for i in range(size)])

    def swap_cores(value):
        return lax.ppermute(value, "dp", [(i, i ^ 1) for i in range(shards)])

    def spread(weight, chunks, split):
        columns = weight.shape[1]
        wide = [(weight, shard), (swap_cores(weight), shard ^ 1)]
        arrivals = []
        for far in range(1, shards // 2):
            source = (shard - 2 * far) % shards
            for chunk in range(chunks):
                width = columns // (groups * chunks) if split else columns // chunks
                block = group * chunks + chunk if split else jnp.int32(chunk)
                sent = weight
                if width != columns:
                    sent = lax.dynamic_slice_in_dim(weight, block * width, width, axis=1)
                got = shift(sent, "dp", shards, 2 * far)
                arrivals.append((chunk, 0, got, source))
                arrivals.append((chunk, 0, swap_cores(got), source ^ 1))
                if split:
                    for other in range(1, groups):
                        passed = shift(got, "grp", groups, other)
                        arrivals.append((chunk, other, passed, source))
                        arrivals.append((chunk, other, swap_cores(passed), source ^ 1))
        return wide, arrivals

    def block_start(chunk, other, chunks, width):
        return (((group - other) % groups) * chunks + chunk) * width

    def blocks_of(wide, arrivals, chunks, split, width):
        blocks = []
        for other in range(groups if split else 1):
            for chunk in range(chunks):
                start = block_start(chunk, other, chunks, width) if split else chunk * width
                items = [(piece, which, start) for piece, which in wide]
                items += [
                    (piece, which, None)
                    for c, o, piece, which in arrivals
                    if c == chunk and o == other
                ]
                blocks.append((start, items))
        return blocks

    positions = part * rows + jnp.arange(rows, dtype=jnp.int32)
    q_tables = rotary_tables(positions, query_gain)
    k_tables = rotary_tables(positions, key_gain)

    kv_columns = key_weight.shape[1]
    q_columns = query_weight.shape[1]
    o_columns = out_weight.shape[1]
    q_chunks, o_chunks = 2, 2
    o_split = o_columns // groups % LANES == 0
    if not o_split or o_columns // groups // o_chunks % LANES:
        o_chunks = 1

    k_wide, k_arrivals = spread(key_weight, 1, True)
    v_wide, v_arrivals = spread(value_weight, 1, False)
    q_wide, q_arrivals = spread(query_weight, q_chunks, True)
    o_wide, o_arrivals = spread(out_weight, o_chunks, o_split)

    width = kv_columns // groups
    keys = run_projection(
        x, None, blocks_of(k_wide, k_arrivals, 1, True, width), width, kv_columns, k_tables, "keys"
    )
    all_keys = [keys] + [shift(keys, "sp", parts, by) for by in range(1, parts)]
    values = run_projection(
        x, None, blocks_of(v_wide, v_arrivals, 1, False, kv_columns), kv_columns, kv_columns, None, "values"
    )
    all_values = [values] + [shift(values, "sp", parts, by) for by in range(1, parts)]
    width = q_columns // (groups * q_chunks)
    queries = run_projection(
        x, None, blocks_of(q_wide, q_arrivals, q_chunks, True, width), width, q_columns, q_tables, "queries"
    )
    attended = attend(queries, all_keys, all_values)
    width = o_columns // ((groups if o_split else 1) * o_chunks)
    pieces = [(piece, which * o_columns) for piece, which in o_wide]
    pieces += [
        (
            piece,
            which * o_columns
            + (block_start(chunk, other, o_chunks, width) if o_split else chunk * width),
        )
        for chunk, other, piece, which in o_arrivals
    ]
    mixed = project_out(attended, pieces, o_columns * shards)
    return mixed.reshape(1, rows, mixed.shape[1])


def solution(mesh):
    sizes = tuple(mesh.shape[name] for name in ("grp", "sp", "dp"))
    in_specs = (
        P(("grp", "dp"), "sp", None),
        P("dp", None),
        P("dp", None),
        P("dp", None),
        P(None, "dp"),
        P(),
        P(),
    )
    out_specs = P(("grp", "dp"), "sp", None)
    return jax.shard_map(
        functools.partial(layer, sizes),
        mesh=mesh,
        in_specs=in_specs,
        out_specs=out_specs,
        check_vma=False,
    )
```
